32 devices in a mesh: sp: 8 (over z, y), tp: 4 (over x, core).
Axes of the slice: x: 2, y: 2, z: 4, core: 2. Of those that a mesh axis runs over, the one named last changes fastest.
Arguments:
- queries: bfloat16 [4096, 1024], P('sp', 'tp'), may hold values from -200 to 200
- keys: bfloat16 [4096, 1024], P('sp', 'tp'), may hold values from -6 to 6
- values: bfloat16 [4096, 1024], P('sp', 'tp'), may hold values from -24 to 24
- cum_gate: float32 [4096, 8], P('sp', 'tp'), may hold values from -414 to 0, as said below
- residual: bfloat16 [4096, 2048], P(('sp', 'tp')), may hold values from -1.5 to 1.5
- w_out: bfloat16 [1024, 2048], replicated, may hold values from -0.1875 to 0.1875
- gain: float32 [2048], replicated, may hold values from 0.1 to 1.9
- w_up: bfloat16 [2048, 8192], P('sp', 'tp'), may hold values from -0.125 to 0.125
- w_down: bfloat16 [8192, 2048], P('tp', 'sp'), may hold values from -0.0625 to 0.0625
Outputs:
- output: bfloat16 [4096, 2048], P(('sp', 'tp'))
The draws below stay inside these ranges and needn't reach their ends.
Inputs may be any that keep to these rules, and one draw needn't show every extreme that they name: Within each head, cum_gate never rises from one position to the next.
All inputs are finite; a program needn't handle non-finite values.
Results may differ from the reference program's by a relative error of at most 0.022.
Values may be sent and summed in bfloat16 or wider, within the bound.
A program may use at most 128 MiB of HBM per device.

```python
import math
import jax
import jax.numpy as jnp
from jax import lax

D = 2048
HEADS = 8
HEAD_DIM = 128
FF = 8192
TOK_DEV = 512
SEQUENCE_TOKENS = 4096
N_TP = 4


def joint_pair(key):
    width = HEADS * HEAD_DIM
    query_key = jax.random.fold_in(key, 101)
    key_key = jax.random.fold_in(key, 202)
    keys = jnp.clip(jax.random.normal(key_key, (SEQUENCE_TOKENS, width), jnp.float32), -6.0, 6.0)
    queries = jnp.clip(2.0 * jax.random.normal(query_key, (SEQUENCE_TOKENS, width), jnp.float32), -12.0, 12.0)
    return (queries, keys)


def draw_queries(key, part):
    return joint_pair(key)[0].astype(jnp.bfloat16)


def draw_keys(key, part):
    return joint_pair(key)[1].astype(jnp.bfloat16)


def draw_cum_gate(key, part):
    shuffle_random_key, gradual_decay_key, quick_decay_key, block_random_key, jitter_random_key, spike_random_key, layer_depth_key = jax.random.split(key, 7)
    order = jax.random.permutation(shuffle_random_key, HEADS)
    slow = order < HEADS // 2
    slow_rate = jax.random.uniform(gradual_decay_key, (HEADS,), jnp.float32, 0.2, 0.6) / SEQUENCE_TOKENS
    fast_rate = 1.0 / jnp.exp(jax.random.uniform(quick_decay_key, (HEADS,), jnp.float32, math.log(30.0), math.log(100.0)))
    rate = jnp.where(slow, slow_rate, fast_rate)
    shards = SEQUENCE_TOKENS // TOK_DEV
    factor = 2.0 ** jax.random.uniform(block_random_key, (shards, HEADS), jnp.float32, -1.0, 1.0)
    token_positions = jnp.arange(SEQUENCE_TOKENS)
    per_row = factor[token_positions // TOK_DEV]
    noise = jax.random.uniform(jitter_random_key, (SEQUENCE_TOKENS, HEADS), jnp.float32, 0.5, 1.5)
    steps = -rate[None, :] * per_row * noise
    spike_events = jax.random.randint(spike_random_key, (3,), 0, SEQUENCE_TOKENS)
    depth = jnp.log(jax.random.uniform(layer_depth_key, (3, HEADS), jnp.float32, 0.6, 0.8))
    match_events = (token_positions[:, None] == spike_events[None, :]).astype(jnp.float32)
    steps = steps + jnp.dot(match_events, depth) * slow.astype(jnp.float32)[None, :]
    return jnp.cumsum(steps, axis=0)


def level_of(own_key, extent, pieces, smallest, top_value):
    level, own = 1.0, jax.random.fold_in(own_key, 6)
    for axis_at, shards_of in pieces:
        heights = jnp.exp(jax.random.uniform(jax.random.fold_in(own, axis_at), (shards_of,), jnp.float32, smallest / len(pieces), top_value / len(pieces)))
        level = level * jnp.repeat(heights, extent[axis_at] // shards_of).reshape([-1 if axis == axis_at else 1 for axis in range(len(extent))])
    return level


def centred(rng, shape, scale, limit, pieces=(), held_as=jnp.bfloat16):
    drawn = jax.random.normal(rng, shape, jnp.float32) * scale
    if len(pieces) > 0:
        drawn = level_of(rng, shape, pieces, -0.22, 0.18) * drawn
    return jnp.clip(drawn, min=-limit, max=limit).astype(held_as)


def setup_inputs(seed: int = 0) -> dict:
    streams_of = jax.random.split(jax.random.key(seed), 10)
    queries = draw_queries(jax.random.fold_in(streams_of[9], 71), 0)
    keys = draw_keys(jax.random.fold_in(streams_of[9], 71), 0)
    values = centred(streams_of[2], (SEQUENCE_TOKENS, HEADS * HEAD_DIM), 4.0, 24.0, ((0, 8), (1, 4)))
    cum_gate = draw_cum_gate(jax.random.fold_in(streams_of[9], 71), 0)
    residual = centred(streams_of[4], (SEQUENCE_TOKENS, D), 0.25, 1.5, ((0, 32),))
    w_out = centred(streams_of[5], (HEADS * HEAD_DIM, D), (HEADS * HEAD_DIM) ** -0.5, 0.1875)
    gain = jnp.clip(1.0 + 0.18 * jax.random.normal(streams_of[6], (D,), jnp.float32), 0.1, 1.9)
    w_up = centred(streams_of[7], (D, FF), D ** -0.5, 0.125, ((0, 8), (1, 4)))
    w_down = centred(streams_of[8], (FF, D), FF ** -0.5, 0.0625, ((0, 4), (1, 8)))
    return dict(queries=queries, keys=keys, values=values, cum_gate=cum_gate, residual=residual, w_out=w_out, gain=gain, w_up=w_up, w_down=w_down)


def reference(queries, keys, values, cum_gate, residual, w_out, gain, w_up, w_down):
    width = HEADS * HEAD_DIM
    q_block = math.gcd(SEQUENCE_TOKENS, 512)
    key_heads = keys.astype(jnp.float32).reshape(SEQUENCE_TOKENS, HEADS, HEAD_DIM)
    value_heads = values.astype(jnp.float32).reshape(SEQUENCE_TOKENS, HEADS, HEAD_DIM)
    key_pos = jnp.arange(SEQUENCE_TOKENS, dtype=jnp.int32)
    gate_rows = cum_gate.T

    def attend(block_index):
        offset = (block_index * q_block).astype(jnp.int32)
        query_blk = lax.dynamic_slice_in_dim(queries, offset, q_block, 0).astype(jnp.float32)
        query_blk = query_blk.reshape(q_block, HEADS, HEAD_DIM)
        gate_blk = lax.dynamic_slice_in_dim(cum_gate, offset, q_block, 0)
        scores = jnp.einsum('qhd,khd->qhk', query_blk, key_heads) * HEAD_DIM ** (-0.5)
        scores = scores + gate_blk[:, :, None] - gate_rows[None, :, :]
        query_pos = offset + jnp.arange(q_block, dtype=jnp.int32)
        scores = jnp.where(key_pos[None, None, :] <= query_pos[:, None, None], scores, -1e+30)
        top = lax.optimization_barrier(jnp.max(scores, axis=-1, keepdims=True))
        weights = jnp.exp(scores - top)
        denom = lax.optimization_barrier(jnp.sum(weights, axis=-1))
        rounded = lax.optimization_barrier(weights.astype(jnp.bfloat16)).astype(jnp.float32)
        numer = jnp.einsum('qhk,khd->qhd', rounded, value_heads)
        return (numer / denom[:, :, None]).reshape(q_block, width).astype(jnp.bfloat16)
    blocks = lax.map(attend, jnp.arange(SEQUENCE_TOKENS // q_block, dtype=jnp.int32))
    attended = blocks.reshape(SEQUENCE_TOKENS, width)
    residual_sum = residual.astype(jnp.float32) + jnp.dot(attended, w_out, preferred_element_type=jnp.float32)
    mean_square = lax.optimization_barrier(jnp.mean(residual_sum * residual_sum, axis=-1, keepdims=True))
    normed = (residual_sum * lax.rsqrt(mean_square + 1e-06) * gain).astype(jnp.bfloat16)
    up_proj = jnp.dot(normed, w_up, preferred_element_type=jnp.float32)
    hidden = jnp.square(jax.nn.relu(up_proj)).astype(jnp.bfloat16)
    group = FF // N_TP
    summed = jnp.zeros((SEQUENCE_TOKENS, D), jnp.float32)
    for index in range(N_TP):
        part_out = jnp.dot(hidden[:, index * group:(index + 1) * group], w_down[index * group:(index + 1) * group], preferred_element_type=jnp.float32).astype(jnp.bfloat16)
        summed = summed + lax.optimization_barrier(part_out).astype(jnp.float32)
    return (residual_sum + summed).astype(jnp.bfloat16)
```

```python
import functools
import math

import jax
import jax.numpy as jnp
from jax import lax
from jax.experimental import pallas as pl
from jax.experimental.pallas import tpu as pltpu
from jax.sharding import PartitionSpec as P

LOG2E = math.log2(math.e)
NEG = -1e30
STAT = 8


class Weights:
    def __init__(self, geo, rcopy, own, at, s_z, s_l, s_y, r):
        self.geo, self.rcopy, self.own, self.at = geo, rcopy, own, at
        self.s_z, self.s_l, self.s_y, self.r = s_z, s_l, s_y, r

    def mate(self, j):
        g = self.geo
        return g.par * g.hz + (g.zi + j) % g.hz

    def far(self, j):
        g = self.geo
        return (1 - g.par) * g.hz + (g.zi + j) % g.hz

    def to_mate(self, j):
        g = self.geo
        z = self.mate(j)
        return self.rcopy(self.own(g.par), self.at(g.me), self.s_z.at[j], self.r.at[g.me], z * g.ny + g.y)

    def to_partner(self):
        g = self.geo
        return self.rcopy(self.own(1 - g.par), self.at(g.me), self.s_z.at[0], self.r.at[g.me], self.far(0) * g.ny + g.y)

    def own_y(self, dy):
        g = self.geo
        return self.rcopy(self.own(g.par), self.at(g.me), self.s_y.at[g.z * g.ny + dy], self.r.at[g.me],
                          g.z * g.ny + (g.y + dy) % g.ny)

    def relay(self, j):
        g = self.geo
        s = self.far(0) * g.ny + g.y
        return self.rcopy(self.at(s), self.at(s), self.s_l.at[j], self.r.at[s], self.mate(j) * g.ny + g.y)

    def forward(self, zs, dy):
        g = self.geo
        s = zs * g.ny + g.y
        return self.rcopy(self.at(s), self.at(s), self.s_y.at[zs * g.ny + dy], self.r.at[s],
                          g.z * g.ny + (g.y + dy) % g.ny)

    def wait(self, s):
        self.rcopy(self.own(0), self.at(s), self.s_z.at[0], self.r.at[s], self.geo.me).wait_recv()

    def order(self, i):
        g = self.geo
        if i == 0:
            return g.z
        if i == 1:
            return self.far(0)
        return self.mate(i - 1) if i <= g.hz else self.far(i - g.hz)

    def service(self, i):
        g = self.geo
        zs = self.order(i)
        self.wait(zs * g.ny + g.y)
        if i == 1:
            for j in range(1, g.hz):
                self.relay(j).start()
        for dy in range(1, g.ny):
            self.forward(zs, dy).start()

    def level_wait(self, i):
        g = self.geo
        zs = self.order(i)
        for dy in range(1, g.ny):
            self.wait(zs * g.ny + (g.y + dy) % g.ny)

    def drain(self):
        g = self.geo
        for j in range(1, g.hz):
            self.to_mate(j).wait_send()
            self.relay(j).wait_send()
        self.to_partner().wait_send()
        for dy in range(1, g.ny):
            self.own_y(dy).wait_send()
            for i in range(1, g.nz):
                self.forward(self.order(i), dy).wait_send()


class Geo:
    pass


def body(
    n_sp, n_tp, heads,
    q_ref, k_ref, v_ref, gate_ref, res_ref, wout_hbm, gain_ref, wup_hbm, wdn_hbm,
    out_ref,
    q_all, k_all, v_all, g_all, o_send, o_recv, t_send, t_recv, st_s, m_s, l_s, acc_s,
    att, att_in, wout, rsum, wu, wd, norm_all, hid, psend, pmate, pcomb, precv,
    q_s, q_r, k_s, k_r, v_s, v_r, g_s, g_r, o_s, o_r, t_s, t_r,
    u_z, u_l, u_y, u_r, d_z, d_l, d_y, d_r,
    a_s, a_r, n_s, n_r, p_s, p_r, x_s, x_r, loc,
):
    ny = n_tp // 2
    nz = n_sp // ny
    hz = nz // 2
    cx = n_tp // 2
    tok, width = q_ref.shape
    hd = width // heads
    rows = tok // n_tp
    group = 2 * n_tp
    half = wu.shape[1]
    up_rows = wup_hbm.shape[0]
    cs = wdn_hbm.shape[1]
    me = lax.axis_index("sp")
    tp = lax.axis_index("tp")
    z, y = me // ny, me % ny
    par, zi = z // hz, z % hz
    x, core = tp // 2, tp % 2
    slot = par * n_tp + tp
    chips = group // 2
    mine = slot // 2
    mate = slot + 1 - 2 * core

    def rcopy(src, dst, ss, rs, sp_to, tp_to=None):
        where = {"sp": sp_to} if tp_to is None else {"sp": sp_to, "tp": tp_to}
        return pltpu.make_async_remote_copy(
            src_ref=src, dst_ref=dst, send_sem=ss, recv_sem=rs,
            device_id=where, device_id_type=pl.DeviceIdType.MESH,
        )

    def place(other):
        return ((other // n_tp) * hz + zi) * ny + y, other % n_tp

    k_all[pl.ds(y, 1)] = k_ref[...][None]
    v_all[pl.ds(y, 1)] = v_ref[...][None]
    g_all[pl.ds(y, 1)] = gate_ref[...][None]
    st_s[...] = jnp.zeros_like(st_s)
    t_recv[...] = jnp.zeros_like(t_recv)

    barrier = pltpu.get_barrier_semaphore()
    for dz in range(1, nz):
        pl.semaphore_signal(barrier, inc=1, device_id={"sp": ((z + dz) % nz) * ny + y},
                            device_id_type=pl.DeviceIdType.MESH)
    for dy in range(1, ny):
        pl.semaphore_signal(barrier, inc=1, device_id={"sp": z * ny + (y + dy) % ny},
                            device_id_type=pl.DeviceIdType.MESH)
    for o in range(1, group):
        sp_to, tp_to = place((slot + o) % group)
        pl.semaphore_signal(barrier, inc=1, device_id={"sp": sp_to, "tp": tp_to},
                            device_id_type=pl.DeviceIdType.MESH)
    with jax.named_scope("bar"):
        pl.semaphore_wait(barrier, nz - 1 + ny - 1 + group - 1)

    geo = Geo()
    geo.nz, geo.ny, geo.hz, geo.me, geo.z, geo.y, geo.par, geo.zi = nz, ny, hz, me, z, y, par, zi
    up = Weights(
        geo, rcopy,
        lambda p: wup_hbm.at[:, pl.ds(pl.multiple_of(p * half, half), half)],
        lambda s: wu.at[pl.ds(pl.multiple_of(s * up_rows, up_rows), up_rows), :],
        u_z, u_l, u_y, u_r,
    )
    dn = Weights(
        geo, rcopy,
        lambda p: wdn_hbm.at[pl.ds(pl.multiple_of(p * half, half), half), :],
        lambda s: wd.at[s],
        d_z, d_l, d_y, d_r,
    )

    def keys_to(dy):
        to = z * ny + (y + dy) % ny
        return (rcopy(k_ref, k_all.at[y], k_s.at[dy], k_r.at[y], to),
                rcopy(gate_ref, g_all.at[y], g_s.at[dy], g_r.at[y], to),
                rcopy(v_ref, v_all.at[y], v_s.at[dy], v_r.at[y], to))

    def keys_wanted(dy):
        return (z + 1 < nz) | ((y + dy) % ny > y)

    def query_to(zk):
        return rcopy(q_ref, q_all.at[z], q_s.at[zk], q_r.at[z], zk * ny + y)

    def part_to(zq):
        to = zq * ny + y
        at = pl.ds(pl.multiple_of(z * STAT, STAT), STAT)
        return (rcopy(o_send.at[zq], o_recv.at[z], o_s.at[zq], o_r.at[z], to),
                rcopy(t_send.at[zq], t_recv.at[at, :], t_s.at[zq], t_r.at[z], to))

    for dy in range(1, ny):
        @pl.when(keys_wanted(dy))
        def _(dy=dy):
            for c in keys_to(dy):
                c.start()
    for zk in range(nz - 1):
        @pl.when(zk < z)
        def _(zk=zk):
            query_to(zk).start()
    local_wout = pltpu.make_async_copy(wout_hbm, wout, loc.at[0])
    local_up = pltpu.make_async_copy(up.own(par), up.at(me), loc.at[1])
    local_dn = pltpu.make_async_copy(dn.own(par), dn.at(me), loc.at[2])
    local_up.start()
    local_dn.start()
    local_wout.start()
    up.to_partner().start()
    for j in range(1, hz):
        up.to_mate(j).start()
    for dy in range(1, ny):
        up.own_y(dy).start()
    for dy in range(1, ny):
        dn.own_y(dy).start()

    scale = hd ** (-0.5) * LOG2E

    def absorb(k, v, gates, diagonal):
        for h in range(heads):
            cols = pl.ds(h * hd, hd)
            rel = (gates[h:h + 1, :] - gate_ref[h:h + 1, 0:1]) * LOG2E
            s = lax.dot_general(q_ref[:, cols], k[:, cols], (((1,), (1,)), ((), ())),
                                preferred_element_type=jnp.float32)
            s = s * scale - rel
            if diagonal:
                qp = lax.broadcasted_iota(jnp.int32, s.shape, 0)
                kp = lax.broadcasted_iota(jnp.int32, s.shape, 1)
                s = jnp.where(kp <= qp, s, NEG)
            top = jnp.max(s, axis=1, keepdims=True)
            if not diagonal:
                old = m_s[:, h:h + 1]
                top = jnp.maximum(old, top)
                fade = jnp.exp2(old - top)
            w = jnp.exp2(s - top)
            total = jnp.sum(w, axis=1, keepdims=True)
            add = jnp.dot(w.astype(jnp.bfloat16), v[:, cols], preferred_element_type=jnp.float32)
            if not diagonal:
                total = l_s[:, h:h + 1] * fade + total
                add = acc_s[:, cols] * fade + add
            m_s[:, h:h + 1] = top
            l_s[:, h:h + 1] = total
            acc_s[:, cols] = add

    def partial(zq):
        for h in range(heads):
            cols = pl.ds(h * hd, hd)
            base = gate_ref[h:h + 1, 0:1] * LOG2E
            ss = []
            for i in range(ny):
                rel = g_all[i, h:h + 1, :] * LOG2E - base
                s = lax.dot_general(q_all[zq, :, cols], k_all[i, :, cols], (((1,), (1,)), ((), ())),
                                    preferred_element_type=jnp.float32)
                ss.append(s * scale - rel)
            top = jnp.max(functools.reduce(jnp.maximum, ss), axis=1, keepdims=True)
            total, add = 0.0, 0.0
            for i in range(ny):
                w = jnp.exp2(ss[i] - top)
                total += jnp.sum(w, axis=1, keepdims=True)
                add += jnp.dot(w.astype(jnp.bfloat16), v_all[i, :, cols], preferred_element_type=jnp.float32)
            o_send[zq, :, cols] = add.astype(jnp.bfloat16)
            st_s[:, h:h + 1] = top - base
            st_s[:, heads + h:heads + h + 1] = total
        t_send[zq] = jnp.transpose(st_s[...])[0:STAT, :]

    with jax.named_scope("diag"):
        absorb(k_ref, v_ref, gate_ref, True)

    for dy in range(1, ny):
        src = (y + dy) % ny

        @pl.when((z + 1 < nz) | (src < y))
        def _(dy=dy, src=src):
            with jax.named_scope("kvwait"):
                for ref, all_, ss, rs in ((k_ref, k_all, k_s, k_r), (gate_ref, g_all, g_s, g_r), (v_ref, v_all, v_s, v_r)):
                    rcopy(ref, all_.at[src], ss.at[0], rs.at[src], me).wait_recv()

            @pl.when(src < y)
            def _():
                with jax.named_scope("absorb"):
                    absorb(k_all.at[src], v_all.at[src], g_all.at[src], False)

    def query_level(i, carry):
        zq = nz - 1 - i

        @pl.when(zq > z)
        def _():
            with jax.named_scope("qwait"):
                rcopy(q_ref, q_all.at[zq], q_s.at[0], q_r.at[zq], me).wait_recv()
            with jax.named_scope("partial"):
                partial(zq)
            for c in part_to(zq):
                c.start()
        return carry

    lax.fori_loop(0, nz, query_level, 0)

    with jax.named_scope("upsvc"):
        for i in range(1, hz + 1):
            up.service(i)

    for zk in range(nz - 1):
        @pl.when(zk < z)
        def _(zk=zk):
            with jax.named_scope("owait"):
                at = pl.ds(zk * STAT, STAT)
                rcopy(o_send.at[0], o_recv.at[zk], o_s.at[0], o_r.at[zk], me).wait_recv()
                rcopy(t_send.at[0], t_recv.at[at, :], t_s.at[0], t_r.at[zk], me).wait_recv()

    @pl.when(z > 0)
    def _():
        st_s[...] = jnp.transpose(t_recv[...])

    for zk in range(nz - 1):
        @pl.when(zk < z)
        def _(zk=zk):
            for h in range(heads):
                cols = pl.ds(h * hd, hd)
                at = zk * STAT + h
                their = st_s[:, at:at + 1] + gate_ref[h:h + 1, 0:1] * LOG2E
                old = m_s[:, h:h + 1]
                top = jnp.maximum(old, their)
                fade, rise = jnp.exp2(old - top), jnp.exp2(their - top)
                m_s[:, h:h + 1] = top
                l_s[:, h:h + 1] = l_s[:, h:h + 1] * fade + st_s[:, at + heads:at + heads + 1] * rise
                acc_s[:, cols] = acc_s[:, cols] * fade + o_recv[zk, :, cols].astype(jnp.float32) * rise

    for h in range(heads):
        cols = pl.ds(h * hd, hd)
        done = (acc_s[:, cols] / l_s[:, h:h + 1]).astype(jnp.bfloat16)
        for j in range(n_tp):
            att[j, :, cols] = done[j * rows:(j + 1) * rows, :]

    def heads_to(o):
        to = (tp + o) % n_tp
        return rcopy(att.at[to], att_in.at[tp], a_s.at[o], a_r.at[tp], me, to)

    for o in range(1, n_tp):
        heads_to(o).start()
    att_in[pl.ds(tp, 1)] = att[pl.ds(tp, 1)]
    local_wout.wait()
    with jax.named_scope("attwait"):
        for o in range(1, n_tp):
            src = (tp + o) % n_tp
            rcopy(att.at[0], att_in.at[src], a_s.at[0], a_r.at[src], me, tp).wait_recv()
    total = res_ref[...].astype(jnp.float32)
    for j in range(n_tp):
        total += jnp.dot(att_in[j], wout[j * width:(j + 1) * width, :], preferred_element_type=jnp.float32)
    rsum[...] = total
    mean_square = jnp.mean(total * total, axis=-1, keepdims=True)
    normed = (total * lax.rsqrt(mean_square + 1e-06) * gain_ref[...]).astype(jnp.bfloat16)

    def block(ref, b):
        at = (b % 2) * chips + b // 2
        return ref.at[pl.ds(pl.multiple_of(at * rows, rows), rows), :]

    block(norm_all, slot)[...] = normed

    def normed_row(src, sem, other):
        sp_to, tp_to = place(other)
        return rcopy(block(norm_all, src), block(norm_all, src), n_s.at[sem], n_r.at[src], sp_to, tp_to)

    def beside(k):
        return par * n_tp + ((x + k) % cx) * 2 + core

    across = (1 - par) * n_tp + tp

    def normed_beside(k):
        return normed_row(slot, k, beside(k))

    def normed_across():
        return normed_row(slot, 0, across)

    def normed_relay(k):
        return normed_row(across, cx + k, beside(k))

    def normed_mate(k):
        return normed_row((slot + 2 * k) % group, chips + k, mate)

    def normed_wait(src):
        rcopy(block(norm_all, src), block(norm_all, src), n_s.at[0], n_r.at[src], me).wait_recv()

    normed_across().start()
    for k in range(1, cx):
        normed_beside(k).start()
    normed_mate(0).start()

    dn.to_partner().start()
    for j in range(1, hz):
        dn.to_mate(j).start()

    with jax.named_scope("upsvc2"):
        for i in range(hz + 1, nz):
            up.service(i)

    with jax.named_scope("normwait_across"):
        normed_wait(across)
    for k in range(1, cx):
        normed_relay(k).start()
    with jax.named_scope("normwait_chip"):
        normed_mate(chips // 2).start()
        for k in range(1, chips):
            if k != chips // 2:
                normed_wait((slot + 2 * k) % group)
                normed_mate(k).start()

    local_up.wait()
    with jax.named_scope("upwait_y"):
        for i in range(nz):
            up.level_wait(i)
    with jax.named_scope("normwait_mate"):
        for k in range(chips):
            normed_wait((mate + 2 * k) % group)

    tile = min(256, half)

    def up_tile(i, carry):
        cols = pl.ds(pl.multiple_of(i * tile, tile), tile)
        u = jnp.maximum(jnp.dot(norm_all[...], wu[:, cols], preferred_element_type=jnp.float32), 0.0)
        hid[:, cols] = (u * u).astype(jnp.bfloat16)
        return carry

    with jax.named_scope("up_mm"):
        lax.fori_loop(0, half // tile, up_tile, 0)

    per = max(1, 128 // cs)
    span = ny * cs

    def part(ref, at, count, zs):
        return ref.at[pl.ds(pl.multiple_of(at * rows, rows), count * rows),
                      pl.ds(pl.multiple_of(zs * span, span), span)]

    def to_mate(zs):
        return rcopy(part(psend, (1 - core) * chips, chips, zs), part(pmate, 0, chips, zs),
                     x_s.at[zs], x_r.at[zs], me, mate % n_tp)

    def partial_to(k, zs):
        chip = (mine + k) % chips
        sp_to, tp_to = place(chip * 2 + core)
        return rcopy(part(pcomb, chip, 1, zs), part(precv, mine, 1, zs), p_s.at[k * nz + zs],
                     p_r.at[mine * nz + zs], sp_to, tp_to)

    def down_level(zs):
        for k in range(ny // per):
            ws = [wd[zs * ny + k * per + i] for i in range(per)]
            w = ws[0] if per == 1 else jnp.concatenate(ws, axis=1)
            cols = pl.ds(pl.multiple_of((zs * ny + k * per) * cs, per * cs), per * cs)
            psend[:, cols] = jnp.dot(hid[...], w, preferred_element_type=jnp.float32).astype(jnp.bfloat16)
        to_mate(zs).start()

    def combine(zs):
        with jax.named_scope("matewait"):
            to_mate(zs).wait_recv()
        both = (part(psend, core * chips, chips, zs)[...].astype(jnp.float32)
                + part(pmate, 0, chips, zs)[...].astype(jnp.float32))
        part(pcomb, 0, chips, zs)[...] = both.astype(jnp.bfloat16)
        for k in range(1, chips):
            partial_to(k, zs).start()

    local_dn.wait()
    for i in range(nz):
        if i + 1 < nz:
            with jax.named_scope("dnwait_z"):
                dn.service(i + 1)
        with jax.named_scope("dnwait_y"):
            dn.level_wait(i)
        with jax.named_scope("down_mm"):
            down_level(dn.order(i))
        if i > 0:
            combine(dn.order(i - 1))
    combine(dn.order(nz - 1))

    total = rsum[...]
    whole_row = lambda ref, at: ref[pl.ds(pl.multiple_of(at * rows, rows), rows), :].astype(jnp.float32)
    total += whole_row(pcomb, mine)
    for k in range(1, chips):
        src = (mine + k) % chips
        with jax.named_scope("partwait"):
            for zs in range(nz):
                rcopy(part(pcomb, src, 1, zs), part(precv, src, 1, zs), p_s.at[0], p_r.at[src * nz + zs], me).wait_recv()
        total += whole_row(precv, src)
    out_ref[...] = total.astype(jnp.bfloat16)

    for dy in range(1, ny):
        @pl.when(keys_wanted(dy))
        def _(dy=dy):
            for c in keys_to(dy):
                c.wait_send()
    for zk in range(nz - 1):
        @pl.when(zk < z)
        def _(zk=zk):
            query_to(zk).wait_send()
    for zq in range(1, nz):
        @pl.when(zq > z)
        def _(zq=zq):
            for c in part_to(zq):
                c.wait_send()
    up.drain()
    dn.drain()
    for o in range(1, n_tp):
        heads_to(o).wait_send()
    normed_across().wait_send()
    for k in range(1, cx):
        normed_beside(k).wait_send()
        normed_relay(k).wait_send()
    for k in range(chips):
        normed_mate(k).wait_send()
    for zs in range(nz):
        to_mate(zs).wait_send()
        for k in range(1, chips):
            partial_to(k, zs).wait_send()


def per_device(n_sp, n_tp, queries, keys, values, cum_gate, residual, w_out, gain, w_up, w_down):
    tok, width = queries.shape
    heads = cum_gate.shape[1]
    rows, features = residual.shape
    ny = n_tp // 2
    nz = n_sp // ny
    hz = nz // 2
    group = 2 * n_tp
    half = w_up.shape[1] // 2
    bf, f32 = jnp.bfloat16, jnp.float32
    assert nz % 2 == 0 and 2 * heads <= STAT
    gates = jnp.pad(cum_gate.T, ((0, 8 - heads), (0, 0)))
    vmem = pl.BlockSpec(memory_space=pltpu.VMEM)
    hbm = pl.BlockSpec(memory_space=pl.ANY)
    dma = lambda n: pltpu.SemaphoreType.DMA((n,))
    lanes = max(128, nz * STAT)
    return pl.pallas_call(
        functools.partial(body, n_sp, n_tp, heads),
        out_shape=jax.ShapeDtypeStruct((rows, features), bf),
        in_specs=[vmem, vmem, vmem, vmem, vmem, hbm, vmem, hbm, hbm],
        out_specs=vmem,
        scratch_shapes=[
            pltpu.VMEM((nz, tok, width), bf),
            pltpu.VMEM((ny, tok, width), bf),
            pltpu.VMEM((ny, tok, width), bf),
            pltpu.VMEM((ny,) + gates.shape, f32),
            pltpu.VMEM((nz, tok, width), bf),
            pltpu.VMEM((nz, tok, width), bf),
            pltpu.VMEM((nz, STAT, tok), f32),
            pltpu.VMEM((lanes, tok), f32),
            pltpu.VMEM((tok, lanes), f32),
            pltpu.VMEM((tok, 128), f32),
            pltpu.VMEM((tok, 128), f32),
            pltpu.VMEM((tok, width), f32),
            pltpu.VMEM((n_tp, rows, width), bf),
            pltpu.VMEM((n_tp, rows, width), bf),
            pltpu.VMEM(w_out.shape, bf),
            pltpu.VMEM((rows, features), f32),
            pltpu.VMEM((n_sp * w_up.shape[0], half), bf),
            pltpu.VMEM((n_sp, half, w_down.shape[1]), bf),
            pltpu.VMEM((group * rows, features), bf),
            pltpu.VMEM((group * rows, half), bf),
            pltpu.VMEM((group * rows, features), bf),
            pltpu.VMEM((n_tp * rows, features), bf),
            pltpu.VMEM((n_tp * rows, features), bf),
            pltpu.VMEM((n_tp * rows, features), bf),
        ]
        + [dma(nz), dma(nz)] + [dma(ny)] * 6 + [dma(nz)] * 4
        + [dma(hz), dma(hz), dma(n_sp), dma(n_sp)] * 2
        + [dma(n_tp), dma(n_tp), dma(group + n_tp), dma(group), dma(n_tp * nz), dma(n_tp * nz), dma(nz), dma(nz), dma(3)],
        compiler_params=pltpu.CompilerParams(
            collective_id=0, has_side_effects=True, vmem_limit_bytes=63 * 1024 * 1024
        ),
    )(queries, keys, values, gates, residual, w_out, gain.reshape(1, -1), w_up, w_down)


def solution(mesh):
    n_sp, n_tp = mesh.shape["sp"], mesh.shape["tp"]
    return jax.shard_map(
        functools.partial(per_device, n_sp, n_tp),
        mesh=mesh,
        in_specs=(
            P("sp", "tp"),
            P("sp", "tp"),
            P("sp", "tp"),
            P("sp", "tp"),
            P(("sp", "tp"), None),
            P(),
            P(),
            P("sp", "tp"),
            P("tp", "sp"),
        ),
        out_specs=P(("sp", "tp"), None),
        check_vma=False,
    )
```

```python
import functools
import math

import jax
import jax.numpy as jnp
from jax import lax
from jax.experimental import pallas as pl
from jax.experimental.pallas import tpu as pltpu
from jax.sharding import PartitionSpec as P

LOG2E = math.log2(math.e)
NEG = -1e30
STAT = 8
CUTS = 2


class Weights:
    def __init__(self, geo, cuts, rcopy, own, at, s_z, s_l, s_y, r):
        self.geo, self.cuts, self.rcopy, self.own, self.at = geo, cuts, rcopy, own, at
        self.s_z, self.s_l, self.s_y, self.r = s_z, s_l, s_y, r

    def mate(self, j):
        g = self.geo
        return g.par * g.hz + (g.zi + j) % g.hz

    def far(self, j):
        g = self.geo
        return (1 - g.par) * g.hz + (g.zi + j) % g.hz

    def send(self, src, s, c, sem, k, z, y):
        return self.rcopy(src, self.at(s, c), sem.at[k * self.cuts + c], self.r.at[s * self.cuts + c], z * self.geo.ny + y)

    def to_mate(self, j, c):
        g = self.geo
        return self.send(self.own(g.par, c), g.me, c, self.s_z, j, self.mate(j), g.y)

    def to_partner(self, c):
        g = self.geo
        return self.send(self.own(1 - g.par, c), g.me, c, self.s_z, 0, self.far(0), g.y)

    def own_y(self, dy, c):
        g = self.geo
        return self.send(self.own(g.par, c), g.me, c, self.s_y, g.z * g.ny + dy, g.z, (g.y + dy) % g.ny)

    def relay(self, j, c):
        g = self.geo
        s = self.far(0) * g.ny + g.y
        return self.send(self.at(s, c), s, c, self.s_l, j, self.mate(j), g.y)

    def forward(self, zs, dy, c):
        g = self.geo
        s = zs * g.ny + g.y
        return self.send(self.at(s, c), s, c, self.s_y, zs * g.ny + dy, g.z, (g.y + dy) % g.ny)

    def wait(self, s, c):
        self.rcopy(self.own(0, c), self.at(s, c), self.s_z.at[0], self.r.at[s * self.cuts + c], self.geo.me).wait_recv()

    def order(self, i):
        g = self.geo
        return self.mate(i) if i < g.hz else self.far(i - g.hz)

    def service(self, i, c):
        g = self.geo
        zs = self.order(i)
        self.wait(zs * g.ny + g.y, c)
        if i == g.hz:
            for j in range(1, g.hz):
                self.relay(j, c).start()
        for dy in range(1, g.ny):
            self.forward(zs, dy, c).start()

    def drain(self):
        g = self.geo
        for c in range(self.cuts):
            for j in range(1, g.hz):
                self.to_mate(j, c).wait_send()
                self.relay(j, c).wait_send()
            self.to_partner(c).wait_send()
            for dy in range(1, g.ny):
                self.own_y(dy, c).wait_send()
                for i in range(1, g.nz):
                    self.forward(self.order(i), dy, c).wait_send()


class Geo:
    pass


def body(
    n_sp, n_tp, heads,
    q_ref, k_ref, v_ref, gate_ref, res_ref, wout_hbm, gain_ref, wup_hbm, wdn_hbm,
    out_ref,
    q_all, k_all, v_all, g_all, o_send, o_recv, t_send, t_recv, st_s, m_s, l_s, acc_s,
    att, att_in, wout, rsum, wu, wd, norm_all, hid, psend, pmate, pcomb, precv, pfar, pback,
    q_s, q_r, k_s, k_r, v_s, v_r, g_s, g_r, o_s, o_r, t_s, t_r,
    u_z, u_l, u_y, u_r, d_z, d_l, d_y, d_r,
    a_s, a_r, n_s, n_r, p_s, p_r, x_s, x_r, f_s, f_r, loc,
):
    ny = n_tp // 2
    nz = n_sp // ny
    hz = nz // 2
    cx = n_tp // 2
    tok, width = q_ref.shape
    hd = width // heads
    rows = tok // n_tp
    group = 2 * n_tp
    half = wu.shape[1]
    up_rows = wup_hbm.shape[0]
    cs = wdn_hbm.shape[1]
    me = lax.axis_index("sp")
    tp = lax.axis_index("tp")
    z, y = me // ny, me % ny
    par, zi = z // hz, z % hz
    x, core = tp // 2, tp % 2
    slot = par * n_tp + tp
    chips = group // 2
    mine = slot // 2
    mate = slot + 1 - 2 * core

    def rcopy(src, dst, ss, rs, sp_to, tp_to=None):
        where = {"sp": sp_to} if tp_to is None else {"sp": sp_to, "tp": tp_to}
        return pltpu.make_async_remote_copy(
            src_ref=src, dst_ref=dst, send_sem=ss, recv_sem=rs,
            device_id=where, device_id_type=pl.DeviceIdType.MESH,
        )

    def place(other):
        return ((other // n_tp) * hz + zi) * ny + y, other % n_tp

    k_all[pl.ds(y, 1)] = k_ref[...][None]
    v_all[pl.ds(y, 1)] = v_ref[...][None]
    g_all[pl.ds(y, 1)] = gate_ref[...][None]
    st_s[...] = jnp.zeros_like(st_s)
    t_recv[...] = jnp.zeros_like(t_recv)

    barrier = pltpu.get_barrier_semaphore()
    for dz in range(1, nz):
        pl.semaphore_signal(barrier, inc=1, device_id={"sp": ((z + dz) % nz) * ny + y},
                            device_id_type=pl.DeviceIdType.MESH)
    for dy in range(1, ny):
        pl.semaphore_signal(barrier, inc=1, device_id={"sp": z * ny + (y + dy) % ny},
                            device_id_type=pl.DeviceIdType.MESH)
    for o in range(1, group):
        sp_to, tp_to = place((slot + o) % group)
        pl.semaphore_signal(barrier, inc=1, device_id={"sp": sp_to, "tp": tp_to},
                            device_id_type=pl.DeviceIdType.MESH)
    with jax.named_scope("bar"):
        pl.semaphore_wait(barrier, nz - 1 + ny - 1 + group - 1)

    geo = Geo()
    geo.nz, geo.ny, geo.hz, geo.me, geo.z, geo.y, geo.par, geo.zi = nz, ny, hz, me, z, y, par, zi
    cuts = CUTS
    upc, dnc = up_rows // cuts, half // cuts
    up = Weights(
        geo, cuts, rcopy,
        lambda p, c: wup_hbm.at[pl.ds(c * upc, upc), pl.ds(pl.multiple_of(p * half, half), half)],
        lambda s, c: wu.at[pl.ds(pl.multiple_of(s * up_rows + c * upc, upc), upc), :],
        u_z, u_l, u_y, u_r,
    )
    dn = Weights(
        geo, cuts, rcopy,
        lambda p, c: wdn_hbm.at[pl.ds(pl.multiple_of(p * half + c * dnc, dnc), dnc), :],
        lambda s, c: wd.at[s, pl.ds(c * dnc, dnc), :],
        d_z, d_l, d_y, d_r,
    )

    def keys_to(dy):
        to = z * ny + (y + dy) % ny
        return (rcopy(k_ref, k_all.at[y], k_s.at[dy], k_r.at[y], to),
                rcopy(gate_ref, g_all.at[y], g_s.at[dy], g_r.at[y], to),
                rcopy(v_ref, v_all.at[y], v_s.at[dy], v_r.at[y], to))

    def keys_wanted(dy):
        return (z + 1 < nz) | ((y + dy) % ny > y)

    def query_first():
        return rcopy(q_ref, q_all.at[z], q_s.at[z], q_r.at[z], me - ny)

    def query_on(zq):
        return rcopy(q_all.at[zq], q_all.at[zq], q_s.at[zq], q_r.at[zq], me - ny)

    def query_wait(zq):
        rcopy(q_ref, q_all.at[zq], q_s.at[0], q_r.at[zq], me).wait_recv()

    def part_to(zq):
        to = zq * ny + y
        at = pl.ds(pl.multiple_of(z * STAT, STAT), STAT)
        return (rcopy(o_send.at[zq], o_recv.at[z], o_s.at[zq], o_r.at[z], to),
                rcopy(t_send.at[zq], t_recv.at[at, :], t_s.at[zq], t_r.at[z], to))

    for dy in range(1, ny):
        @pl.when(keys_wanted(dy))
        def _(dy=dy):
            for c in keys_to(dy):
                c.start()
    @pl.when(z > 0)
    def _():
        query_first().start()
    local_wout = pltpu.make_async_copy(wout_hbm, wout, loc.at[0])
    local_up = pltpu.make_async_copy(
        wup_hbm.at[:, pl.ds(pl.multiple_of(par * half, half), half)],
        wu.at[pl.ds(pl.multiple_of(me * up_rows, up_rows), up_rows), :], loc.at[1])
    local_dn = pltpu.make_async_copy(
        wdn_hbm.at[pl.ds(pl.multiple_of(par * half, half), half), :], wd.at[me], loc.at[2])

    def direct_mates(w, upward):
        for j in range(1, hz):
            @pl.when((w.mate(j) > z) if upward else (w.mate(j) < z))
            def _(j=j):
                for c in range(cuts):
                    w.to_mate(j, c).start()

    def direct_partner(w, upward, chunks):
        @pl.when(par == (0 if upward else 1))
        def _():
            for c in chunks:
                w.to_partner(c).start()

    every = range(cuts)
    direct_partner(up, True, every)
    direct_mates(up, True)
    local_up.start()
    local_dn.start()
    local_wout.start()
    for w in (up, dn):
        for dy in range(1, ny):
            for c in every:
                w.own_y(dy, c).start()

    scale = hd ** (-0.5) * LOG2E

    def absorb(k, v, gates, diagonal):
        for h in range(heads):
            cols = pl.ds(h * hd, hd)
            rel = (gates[h:h + 1, :] - gate_ref[h:h + 1, 0:1]) * LOG2E
            s = lax.dot_general(q_ref[:, cols], k[:, cols], (((1,), (1,)), ((), ())),
                                preferred_element_type=jnp.float32)
            s = s * scale - rel
            if diagonal:
                qp = lax.broadcasted_iota(jnp.int32, s.shape, 0)
                kp = lax.broadcasted_iota(jnp.int32, s.shape, 1)
                s = jnp.where(kp <= qp, s, NEG)
            top = jnp.max(s, axis=1, keepdims=True)
            if not diagonal:
                old = m_s[:, h:h + 1]
                top = jnp.maximum(old, top)
                fade = jnp.exp2(old - top)
            w = jnp.exp2(s - top)
            total = jnp.sum(w, axis=1, keepdims=True)
            add = jnp.dot(w.astype(jnp.bfloat16), v[:, cols], preferred_element_type=jnp.float32)
            if not diagonal:
                total = l_s[:, h:h + 1] * fade + total
                add = acc_s[:, cols] * fade + add
            m_s[:, h:h + 1] = top
            l_s[:, h:h + 1] = total
            acc_s[:, cols] = add

    def partial(zq):
        for h in range(heads):
            cols = pl.ds(h * hd, hd)
            base = gate_ref[h:h + 1, 0:1] * LOG2E
            ss = []
            for i in range(ny):
                rel = g_all[i, h:h + 1, :] * LOG2E - base
                s = lax.dot_general(q_all[zq, :, cols], k_all[i, :, cols], (((1,), (1,)), ((), ())),
                                    preferred_element_type=jnp.float32)
                ss.append(s * scale - rel)
            top = jnp.max(functools.reduce(jnp.maximum, ss), axis=1, keepdims=True)
            total, add = 0.0, 0.0
            for i in range(ny):
                w = jnp.exp2(ss[i] - top)
                total += jnp.sum(w, axis=1, keepdims=True)
                add += jnp.dot(w.astype(jnp.bfloat16), v_all[i, :, cols], preferred_element_type=jnp.float32)
            o_send[zq, :, cols] = add.astype(jnp.bfloat16)
            st_s[:, h:h + 1] = top - base
            st_s[:, heads + h:heads + h + 1] = total
        t_send[zq] = jnp.transpose(st_s[...])[0:STAT, :]

    with jax.named_scope("diag"):
        absorb(k_ref, v_ref, gate_ref, True)

    for zq in range(2, nz):
        @pl.when((zq > z) & (z > 0))
        def _(zq=zq):
            with jax.named_scope("qfwd"):
                query_wait(zq)
            query_on(zq).start()
    direct_mates(up, False)
    direct_partner(up, False, every)

    for dy in range(1, ny):
        src = (y + dy) % ny

        @pl.when((z + 1 < nz) | (src < y))
        def _(dy=dy, src=src):
            with jax.named_scope("kvwait"):
                for ref, all_, ss, rs in ((k_ref, k_all, k_s, k_r), (gate_ref, g_all, g_s, g_r), (v_ref, v_all, v_s, v_r)):
                    rcopy(ref, all_.at[src], ss.at[0], rs.at[src], me).wait_recv()

            @pl.when(src < y)
            def _():
                with jax.named_scope("absorb"):
                    absorb(k_all.at[src], v_all.at[src], g_all.at[src], False)

    def query_level(i, carry):
        zq = i + 1

        @pl.when(zq > z)
        def _():
            @pl.when(z == 0)
            def _():
                with jax.named_scope("qwait"):
                    query_wait(zq)
            with jax.named_scope("partial"):
                partial(zq)
            for c in part_to(zq):
                c.start()
        return carry

    lax.fori_loop(0, nz - 1, query_level, 0)

    with jax.named_scope("upsvc"):
        for i in [hz] + list(range(1, hz)):
            for c in every:
                up.service(i, c)
    direct_partner(dn, False, every)
    direct_partner(dn, True, [0])
    for p in range(2):
        @pl.when(par == p)
        def _(p=p):
            direct_mates(dn, p == 1)

    for zk in range(nz - 1):
        @pl.when(zk < z)
        def _(zk=zk):
            with jax.named_scope("owait"):
                at = pl.ds(zk * STAT, STAT)
                rcopy(o_send.at[0], o_recv.at[zk], o_s.at[0], o_r.at[zk], me).wait_recv()
                rcopy(t_send.at[0], t_recv.at[at, :], t_s.at[0], t_r.at[zk], me).wait_recv()

    @pl.when(z > 0)
    def _():
        st_s[...] = jnp.transpose(t_recv[...])

    for zk in range(nz - 1):
        @pl.when(zk < z)
        def _(zk=zk):
            for h in range(heads):
                cols = pl.ds(h * hd, hd)
                at = zk * STAT + h
                their = st_s[:, at:at + 1] + gate_ref[h:h + 1, 0:1] * LOG2E
                old = m_s[:, h:h + 1]
                top = jnp.maximum(old, their)
                fade, rise = jnp.exp2(old - top), jnp.exp2(their - top)
                m_s[:, h:h + 1] = top
                l_s[:, h:h + 1] = l_s[:, h:h + 1] * fade + st_s[:, at + heads:at + heads + 1] * rise
                acc_s[:, cols] = acc_s[:, cols] * fade + o_recv[zk, :, cols].astype(jnp.float32) * rise

    for h in range(heads):
        cols = pl.ds(h * hd, hd)
        done = (acc_s[:, cols] / l_s[:, h:h + 1]).astype(jnp.bfloat16)
        for j in range(n_tp):
            att[j, :, cols] = done[j * rows:(j + 1) * rows, :]

    def heads_to(o):
        to = (tp + o) % n_tp
        return rcopy(att.at[to], att_in.at[tp], a_s.at[o], a_r.at[tp], me, to)

    for o in range(1, n_tp):
        heads_to(o).start()
    att_in[pl.ds(tp, 1)] = att[pl.ds(tp, 1)]
    local_wout.wait()
    with jax.named_scope("attwait"):
        for o in range(1, n_tp):
            src = (tp + o) % n_tp
            rcopy(att.at[0], att_in.at[src], a_s.at[0], a_r.at[src], me, tp).wait_recv()
    total = res_ref[...].astype(jnp.float32)
    for j in range(n_tp):
        total += jnp.dot(att_in[j], wout[j * width:(j + 1) * width, :], preferred_element_type=jnp.float32)
    rsum[...] = total
    mean_square = jnp.mean(total * total, axis=-1, keepdims=True)
    normed = (total * lax.rsqrt(mean_square + 1e-06) * gain_ref[...]).astype(jnp.bfloat16)

    def block(ref, b):
        at = (b % 2) * chips + b // 2
        return ref.at[pl.ds(pl.multiple_of(at * rows, rows), rows), :]

    block(norm_all, slot)[...] = normed
    strips = 2
    strip = norm_all.shape[1] // strips

    def strip_of(b, c):
        at = (b % 2) * chips + b // 2
        return norm_all.at[pl.ds(pl.multiple_of(at * rows, rows), rows), pl.ds(c * strip, strip)]

    def normed_row(src, sem, other, c):
        sp_to, tp_to = place(other)
        return rcopy(strip_of(src, c), strip_of(src, c), n_s.at[sem * strips + c], n_r.at[src * strips + c], sp_to, tp_to)

    def beside(k):
        return par * n_tp + ((x + k) % cx) * 2 + core

    across = (1 - par) * n_tp + tp

    def normed_beside(k, c):
        return normed_row(slot, k, beside(k), c)

    def normed_across(c):
        return normed_row(slot, 0, across, c)

    def normed_relay(k, c):
        return normed_row(across, cx + k, beside(k), c)

    def normed_mate(k, c):
        return normed_row((slot + 2 * k) % group, chips + k, mate, c)

    def normed_wait(src, c):
        rcopy(strip_of(src, c), strip_of(src, c), n_s.at[0], n_r.at[src * strips + c], me).wait_recv()

    for c in range(strips):
        normed_across(c).start()
    for c in range(strips):
        for k in range(1, cx):
            normed_beside(k, c).start()
    for c in range(strips):
        normed_mate(0, c).start()
    direct_partner(dn, True, range(1, cuts))
    for p in range(2):
        @pl.when(par == p)
        def _(p=p):
            direct_mates(dn, p == 0)

    with jax.named_scope("upsvc2"):
        for i in range(hz + 1, nz):
            for c in every:
                up.service(i, c)

    def dn_service(i, chunks, name):
        for c in chunks:
            with jax.named_scope(name):
                dn.service(i, c)

    def dn_mates(soon):
        for j in range(1, hz):
            zs = dn.mate(j)

            @pl.when((zs < z) == ((par == 1) == soon))
            def _(j=j):
                dn_service(j, every, "dnsvc_mate")

    dn_service(hz, [0], "dnsvc_part0")

    @pl.when(par == 0)
    def _():
        dn_service(hz, range(1, cuts), "dnsvc_part1")
    dn_mates(True)

    for c in range(strips):
        with jax.named_scope("normwait_across"):
            normed_wait(across, c)
        for k in range(1, cx):
            normed_relay(k, c).start()
        normed_mate(chips // 2, c).start()
    for near in (True, False):
        for k in range(1, cx):
            for c in range(strips):
                b = beside(k) if near else (1 - par) * n_tp + ((x + k) % cx) * 2 + core
                with jax.named_scope("normwait_chip"):
                    normed_wait(b, c)
                normed_row(b, chips + (b // 2 - mine + chips) % chips, mate, c).start()

    dn_mates(False)
    dn_service(hz + 1, [0], "dnsvc_far0") if hz > 1 else None
    local_up.wait()
    with jax.named_scope("upwait_y"):
        for s in range(n_sp):
            @pl.when(s % ny != y)
            def _(s=s):
                for c in every:
                    up.wait(s, c)
    with jax.named_scope("normwait_mate"):
        for k in range(chips):
            for c in range(strips):
                normed_wait((mate + 2 * k) % group, c)

    tile = min(256, half)

    def up_tile(i, carry):
        cols = pl.ds(pl.multiple_of(i * tile, tile), tile)
        u = jnp.maximum(jnp.dot(norm_all[...], wu[:, cols], preferred_element_type=jnp.float32), 0.0)
        hid[:, cols] = (u * u).astype(jnp.bfloat16)
        return carry

    with jax.named_scope("up_mm"):
        lax.fori_loop(0, half // tile, up_tile, 0)

    per = max(1, 128 // cs)
    nk = ny // per
    span = per * cs

    def part(ref, at, count, c):
        return ref.at[pl.ds(pl.multiple_of(at * rows, rows), count * rows),
                      pl.ds(pl.multiple_of(c * span, span), span)]

    def to_mate(c):
        return rcopy(part(psend, (1 - core) * chips, chips, c), part(pmate, 0, chips, c),
                     x_s.at[c], x_r.at[c], me, mate % n_tp)

    def part_beside(k, pz, c):
        xd = (x + k) % cx
        return rcopy(part(pcomb, pz * cx + xd, 1, c), part(precv, x * 2 + pz, 1, c), p_s.at[(k * 2 + pz) * nz * nk + c],
                     p_r.at[(x * 2 + pz) * nz * nk + c], me, xd * 2 + core)

    def part_across(c):
        sp_to, tp_to = place(across)
        return rcopy(part(pfar, 0, 1, c), part(pback, 0, 1, c), f_s.at[c], f_r.at[c], sp_to, tp_to)

    def down_piece(c):
        ws = [wd[c * per + i] for i in range(per)]
        w = ws[0] if per == 1 else jnp.concatenate(ws, axis=1)
        cols = pl.ds(pl.multiple_of(c * span, span), span)
        m = hid.shape[0] // 2
        for a in range(2):
            psend[a * m:(a + 1) * m, cols] = jnp.dot(
                hid[a * m:(a + 1) * m, :], w, preferred_element_type=jnp.float32).astype(jnp.bfloat16)
        to_mate(c).start()

    def combine(c):
        with jax.named_scope("matewait"):
            to_mate(c).wait_recv()
        both = (part(psend, core * chips, chips, c)[...].astype(jnp.float32)
                + part(pmate, 0, chips, c)[...].astype(jnp.float32))
        part(pcomb, 0, chips, c)[...] = both.astype(jnp.bfloat16)
        for pz in range(2):
            for k in range(1, cx):
                part_beside(k, (1 - par + pz) % 2, c).start()

    def reduce(c):
        cols = pl.ds(pl.multiple_of(c * span, span), span)
        for far in (True, False):
            pz = 1 - par if far else par
            total = part(pcomb, pz * cx + x, 1, c)[...].astype(jnp.float32)
            for k in range(1, cx):
                xs = (x + k) % cx
                with jax.named_scope("besidewait"):
                    rcopy(part(pcomb, 0, 1, c), part(precv, xs * 2 + pz, 1, c), p_s.at[0],
                          p_r.at[(xs * 2 + pz) * nz * nk + c], me).wait_recv()
                total += part(precv, xs * 2 + pz, 1, c)[...].astype(jnp.float32)
            if far:
                pfar[:, cols] = total.astype(jnp.bfloat16)
                part_across(c).start()
            else:
                rsum[:, cols] += total

    def finish(c):
        cols = pl.ds(pl.multiple_of(c * span, span), span)
        with jax.named_scope("acrosswait"):
            part_across(c).wait_recv()
        out_ref[:, cols] = (rsum[:, cols] + pback[:, cols].astype(jnp.float32)).astype(jnp.bfloat16)

    local_dn.wait()

    @pl.when(par == 1)
    def _():
        dn_service(hz, range(1, cuts), "dnsvc_part1")
    late = [(hz + 1, c) for c in range(1, cuts)] + [(i, c) for i in range(hz + 2, nz) for c in every]
    pieces = []
    for i in range(nz):
        zs = dn.order(i)
        for k in range(nk):
            c = zs * nk + (y // per + k) % nk
            if i >= hz - 1 and k == 0:
                for j, cut in [t for t in late if t[0] == i + 1]:
                    dn_service(j, [cut], "dnsvc_far")
            with jax.named_scope("dnwait_y"):
                for o in range(per):
                    s = c * per + o

                    @pl.when(s % ny != y)
                    def _(s=s):
                        for cut in every:
                            dn.wait(s, cut)
            with jax.named_scope("down_mm"):
                down_piece(c)
            pieces.append(c)
            n = len(pieces)
            if n > 1:
                combine(pieces[n - 2])
            if n > 3:
                reduce(pieces[n - 4])
    n = len(pieces)
    combine(pieces[n - 1])
    for c in pieces[max(0, n - 3):]:
        reduce(c)
    for c in pieces:
        finish(c)

    for dy in range(1, ny):
        @pl.when(keys_wanted(dy))
        def _(dy=dy):
            for c in keys_to(dy):
                c.wait_send()
    @pl.when(z > 0)
    def _():
        query_first().wait_send()
    for zq in range(2, nz):
        @pl.when((zq > z) & (z > 0))
        def _(zq=zq):
            query_on(zq).wait_send()
    for zq in range(1, nz):
        @pl.when(zq > z)
        def _(zq=zq):
            for c in part_to(zq):
                c.wait_send()
    up.drain()
    dn.drain()
    for o in range(1, n_tp):
        heads_to(o).wait_send()
    for c in range(strips):
        normed_across(c).wait_send()
        for k in range(1, cx):
            normed_beside(k, c).wait_send()
            normed_relay(k, c).wait_send()
        for k in range(chips):
            normed_mate(k, c).wait_send()
    for c in range(nz * nk):
        to_mate(c).wait_send()
        part_across(c).wait_send()
        for pz in range(2):
            for k in range(1, cx):
                part_beside(k, pz, c).wait_send()


def per_device(n_sp, n_tp, queries, keys, values, cum_gate, residual, w_out, gain, w_up, w_down):
    tok, width = queries.shape
    heads = cum_gate.shape[1]
    rows, features = residual.shape
    ny = n_tp // 2
    nz = n_sp // ny
    hz = nz // 2
    group = 2 * n_tp
    half = w_up.shape[1] // 2
    bf, f32 = jnp.bfloat16, jnp.float32
    assert nz % 2 == 0 and 2 * heads <= STAT
    gates = jnp.pad(cum_gate.T, ((0, 8 - heads), (0, 0)))
    vmem = pl.BlockSpec(memory_space=pltpu.VMEM)
    hbm = pl.BlockSpec(memory_space=pl.ANY)
    dma = lambda n: pltpu.SemaphoreType.DMA((n,))
    lanes = max(128, nz * STAT)
    pieces = nz * (ny // max(1, 128 // w_down.shape[1]))
    return pl.pallas_call(
        functools.partial(body, n_sp, n_tp, heads),
        out_shape=jax.ShapeDtypeStruct((rows, features), bf),
        in_specs=[vmem, vmem, vmem, vmem, vmem, hbm, vmem, hbm, hbm],
        out_specs=vmem,
        scratch_shapes=[
            pltpu.VMEM((nz, tok, width), bf),
            pltpu.VMEM((ny, tok, width), bf),
            pltpu.VMEM((ny, tok, width), bf),
            pltpu.VMEM((ny,) + gates.shape, f32),
            pltpu.VMEM((nz, tok, width), bf),
            pltpu.VMEM((nz, tok, width), bf),
            pltpu.VMEM((nz, STAT, tok), f32),
            pltpu.VMEM((lanes, tok), f32),
            pltpu.VMEM((tok, lanes), f32),
            pltpu.VMEM((tok, 128), f32),
            pltpu.VMEM((tok, 128), f32),
            pltpu.VMEM((tok, width), f32),
            pltpu.VMEM((n_tp, rows, width), bf),
            pltpu.VMEM((n_tp, rows, width), bf),
            pltpu.VMEM(w_out.shape, bf),
            pltpu.VMEM((rows, features), f32),
            pltpu.VMEM((n_sp * w_up.shape[0], half), bf),
            pltpu.VMEM((n_sp, half, w_down.shape[1]), bf),
            pltpu.VMEM((group * rows, features), bf),
            pltpu.VMEM((group * rows, half), bf),
            pltpu.VMEM((group * rows, features), bf),
            pltpu.VMEM((n_tp * rows, features), bf),
            pltpu.VMEM((n_tp * rows, features), bf),
            pltpu.VMEM((n_tp * rows, features), bf),
            pltpu.VMEM((rows, features), bf),
            pltpu.VMEM((rows, features), bf),
        ]
        + [dma(nz), dma(nz)] + [dma(ny)] * 6 + [dma(nz)] * 4
        + [dma(hz * CUTS), dma(hz * CUTS), dma(n_sp * CUTS), dma(n_sp * CUTS)] * 2
        + [dma(n_tp), dma(n_tp), dma(2 * group), dma(2 * group)]
        + [dma(n_tp * pieces), dma(n_tp * pieces)] + [dma(pieces)] * 4 + [dma(3)],
        compiler_params=pltpu.CompilerParams(
            collective_id=0, has_side_effects=True, vmem_limit_bytes=63 * 1024 * 1024
        ),
    )(queries, keys, values, gates, residual, w_out, gain.reshape(1, -1), w_up, w_down)


def solution(mesh):
    n_sp, n_tp = mesh.shape["sp"], mesh.shape["tp"]
    return jax.shard_map(
        functools.partial(per_device, n_sp, n_tp),
        mesh=mesh,
        in_specs=(
            P("sp", "tp"),
            P("sp", "tp"),
            P("sp", "tp"),
            P("sp", "tp"),
            P(("sp", "tp"), None),
            P(),
            P(),
            P("sp", "tp"),
            P("tp", "sp"),
        ),
        out_specs=P(("sp", "tp"), None),
        check_vma=False,
    )
```

```python
import functools
import math

import jax
import jax.numpy as jnp
from jax import lax
from jax.experimental import pallas as pl
from jax.experimental.pallas import tpu as pltpu
from jax.sharding import PartitionSpec as P

LOG2E = math.log2(math.e)
NEG = -1e30
STAT = 8


PLAN = dict(
    up_part=[0, 0, 2, 2],
    up_mate=[2, 1, 0, 1],
    dn_part0=[4, 2, 3, 3],
    dn_part1=[6, 6, 5, 6],
    dn_mate=[6, 5, 5, 5],
    s_up_mate=[1, 1, 0, 0],
    s_part0=[2, 2, 3, 3],
    s_part1=[5, 5, 5, 5],
    s_mate=[5, 5, 3, 5],
    s_far0=[5, 5, 5, 5],
    gates=[1, 0],
    style=[1],
    lag=[3],
    cuts=[4],
    strips=[4],
    own_y=[0],
)


class Weights:
    def __init__(self, geo, cuts, rcopy, own, at, s_z, s_l, s_y, r):
        self.geo, self.cuts, self.rcopy, self.own, self.at = geo, cuts, rcopy, own, at
        self.s_z, self.s_l, self.s_y, self.r = s_z, s_l, s_y, r

    def mate(self, j):
        g = self.geo
        return g.par * g.hz + (g.zi + j) % g.hz

    def far(self, j):
        g = self.geo
        return (1 - g.par) * g.hz + (g.zi + j) % g.hz

    def send(self, src, s, c, sem, k, z, y):
        return self.rcopy(src, self.at(s, c), sem.at[k * self.cuts + c], self.r.at[s * self.cuts + c], z * self.geo.ny + y)

    def to_mate(self, j, c):
        g = self.geo
        return self.send(self.own(g.par, c), g.me, c, self.s_z, j, self.mate(j), g.y)

    def to_partner(self, c):
        g = self.geo
        return self.send(self.own(1 - g.par, c), g.me, c, self.s_z, 0, self.far(0), g.y)

    def own_y(self, dy, c):
        g = self.geo
        return self.send(self.own(g.par, c), g.me, c, self.s_y, g.z * g.ny + dy, g.z, (g.y + dy) % g.ny)

    def relay(self, j, c):
        g = self.geo
        s = self.far(0) * g.ny + g.y
        return self.send(self.at(s, c), s, c, self.s_l, j, self.mate(j), g.y)

    def forward(self, zs, dy, c):
        g = self.geo
        s = zs * g.ny + g.y
        return self.send(self.at(s, c), s, c, self.s_y, zs * g.ny + dy, g.z, (g.y + dy) % g.ny)

    def wait(self, s, c):
        self.rcopy(self.own(0, c), self.at(s, c), self.s_z.at[0], self.r.at[s * self.cuts + c], self.geo.me).wait_recv()

    def order(self, i):
        g = self.geo
        return self.mate(i) if i < g.hz else self.far(i - g.hz)

    def service(self, i, c):
        g = self.geo
        zs = self.order(i)
        self.wait(zs * g.ny + g.y, c)
        if i == g.hz:
            for j in range(1, g.hz):
                self.relay(j, c).start()
        for dy in range(1, g.ny):
            self.forward(zs, dy, c).start()

    def drain(self):
        g = self.geo
        for c in range(self.cuts):
            for j in range(1, g.hz):
                self.to_mate(j, c).wait_send()
                self.relay(j, c).wait_send()
            self.to_partner(c).wait_send()
            for dy in range(1, g.ny):
                self.own_y(dy, c).wait_send()
                for i in range(1, g.nz):
                    self.forward(self.order(i), dy, c).wait_send()


class Geo:
    pass


def body(
    n_sp, n_tp, heads,
    q_ref, k_ref, v_ref, gate_ref, res_ref, wout_hbm, gain_ref, wup_hbm, wdn_hbm,
    out_ref,
    q_all, k_all, v_all, g_all, o_send, o_recv, t_send, t_recv, o_mid, t_mid, t_own, st_s, m_s, l_s, acc_s,
    att, att_in, wout, rsum, wu, wd, norm_all, hid, psend, pmate, pcomb, precv, pfar, pback,
    q_s, q_r, k_s, k_r, v_s, v_r, g_s, g_r, o_s, o_r, t_s, t_r, om_r, tm_r,
    u_z, u_l, u_y, u_r, d_z, d_l, d_y, d_r,
    a_s, a_r, n_s, n_r, p_s, p_r, x_s, x_r, f_s, f_r, loc, go,
):
    ny = n_tp // 2
    nz = n_sp // ny
    hz = nz // 2
    cx = n_tp // 2
    tok, width = q_ref.shape
    hd = width // heads
    rows = tok // n_tp
    group = 2 * n_tp
    half = wu.shape[1]
    up_rows = wup_hbm.shape[0]
    cs = wdn_hbm.shape[1]
    me = lax.axis_index("sp")
    tp = lax.axis_index("tp")
    z, y = me // ny, me % ny
    par, zi = z // hz, z % hz
    x, core = tp // 2, tp % 2
    slot = par * n_tp + tp
    chips = group // 2
    mine = slot // 2
    mate = slot + 1 - 2 * core

    def rcopy(src, dst, ss, rs, sp_to, tp_to=None):
        where = {"sp": sp_to} if tp_to is None else {"sp": sp_to, "tp": tp_to}
        return pltpu.make_async_remote_copy(
            src_ref=src, dst_ref=dst, send_sem=ss, recv_sem=rs,
            device_id=where, device_id_type=pl.DeviceIdType.MESH,
        )

    def place(other):
        return ((other // n_tp) * hz + zi) * ny + y, other % n_tp

    k_all[pl.ds(y, 1)] = k_ref[...][None]
    v_all[pl.ds(y, 1)] = v_ref[...][None]
    g_all[pl.ds(y, 1)] = gate_ref[...][None]
    st_s[...] = jnp.zeros_like(st_s)
    t_recv[...] = jnp.zeros_like(t_recv)
    t_mid[...] = jnp.zeros_like(t_mid)
    t_own[...] = jnp.zeros_like(t_own)

    barrier = pltpu.get_barrier_semaphore()
    far_mates = [(s, mate % n_tp) for j in range(1, hz) for s in [(par * hz + (zi + j) % hz) * ny + y]]
    for dz in range(1, nz):
        pl.semaphore_signal(barrier, inc=1, device_id={"sp": ((z + dz) % nz) * ny + y},
                            device_id_type=pl.DeviceIdType.MESH)
    for sp_to, tp_to in far_mates:
        pl.semaphore_signal(barrier, inc=1, device_id={"sp": sp_to, "tp": tp_to},
                            device_id_type=pl.DeviceIdType.MESH)
    for dy in range(1, ny):
        pl.semaphore_signal(barrier, inc=1, device_id={"sp": z * ny + (y + dy) % ny},
                            device_id_type=pl.DeviceIdType.MESH)
    for o in range(1, group):
        sp_to, tp_to = place((slot + o) % group)
        pl.semaphore_signal(barrier, inc=1, device_id={"sp": sp_to, "tp": tp_to},
                            device_id_type=pl.DeviceIdType.MESH)
    with jax.named_scope("bar"):
        pl.semaphore_wait(barrier, nz - 1 + hz - 1 + ny - 1 + group - 1)

    geo = Geo()
    geo.nz, geo.ny, geo.hz, geo.me, geo.z, geo.y, geo.par, geo.zi = nz, ny, hz, me, z, y, par, zi
    cuts = PLAN["cuts"][0]
    upc, dnc = up_rows // cuts, half // cuts
    up = Weights(
        geo, cuts, rcopy,
        lambda p, c: wup_hbm.at[pl.ds(c * upc, upc), pl.ds(pl.multiple_of(p * half, half), half)],
        lambda s, c: wu.at[pl.ds(pl.multiple_of(s * up_rows + c * upc, upc), upc), :],
        u_z, u_l, u_y, u_r,
    )
    dn = Weights(
        geo, cuts, rcopy,
        lambda p, c: wdn_hbm.at[pl.ds(pl.multiple_of(p * half + c * dnc, dnc), dnc), :],
        lambda s, c: wd.at[s, pl.ds(c * dnc, dnc), :],
        d_z, d_l, d_y, d_r,
    )

    def keys_to(dy):
        to = z * ny + (y + dy) % ny
        return (rcopy(k_ref, k_all.at[y], k_s.at[dy], k_r.at[y], to),
                rcopy(gate_ref, g_all.at[y], g_s.at[dy], g_r.at[y], to),
                rcopy(v_ref, v_all.at[y], v_s.at[dy], v_r.at[y], to))

    def keys_wanted(dy):
        return (z + 1 < nz) | ((y + dy) % ny > y)

    def query_head(src, zq, h):
        cols = pl.ds(h * hd, hd)
        return rcopy(src.at[:, cols], q_all.at[zq, :, cols], q_s.at[zq * heads + h], q_r.at[zq * heads + h], me - ny)

    def query_first(h):
        return query_head(q_ref, z, h)

    def query_on(zq, h):
        return query_head(q_all.at[zq], zq, h)

    def query_wait(zq, h):
        cols = pl.ds(h * hd, hd)
        rcopy(q_ref.at[:, cols], q_all.at[zq, :, cols], q_s.at[0], q_r.at[zq * heads + h], me).wait_recv()

    def part_copies(zq, o_to, t_to, at, o_sem, t_sem, to):
        rows_at = pl.ds(pl.multiple_of(at * STAT, STAT), STAT)
        return (rcopy(o_send.at[zq], o_to.at[at], o_s.at[zq], o_sem.at[at], to),
                rcopy(t_send.at[zq], t_to.at[rows_at, :], t_s.at[zq], t_sem.at[at], to))

    def part_to(zq):
        return part_copies(zq, o_recv, t_recv, z, o_r, t_r, zq * ny + y)

    def part_inward(zq):
        return part_copies(zq, o_mid, t_mid, zq, om_r, tm_r, me + ny)

    def inward(zq):
        return (par == 0) & (zq >= hz) & (zi < hz - 1)

    def merged(zq):
        return (par == 0) & (zq >= hz) & (zi > 0)

    def part_do(zq, do):
        @pl.when(inward(zq))
        def _():
            for c in part_inward(zq):
                do(c)

        @pl.when(jnp.logical_not(inward(zq)))
        def _():
            for c in part_to(zq):
                do(c)

    for dy in range(1, ny):
        @pl.when(keys_wanted(dy))
        def _(dy=dy):
            for c in keys_to(dy):
                c.start()
    @pl.when(z > 0)
    def _():
        for h in range(heads):
            query_first(h).start()
    local_wout = pltpu.make_async_copy(wout_hbm, wout, loc.at[0])
    local_up = pltpu.make_async_copy(
        wup_hbm.at[:, pl.ds(pl.multiple_of(par * half, half), half)],
        wu.at[pl.ds(pl.multiple_of(me * up_rows, up_rows), up_rows), :], loc.at[1])
    local_dn = pltpu.make_async_copy(
        wdn_hbm.at[pl.ds(pl.multiple_of(par * half, half), half), :], wd.at[me], loc.at[2])

    every = range(cuts)
    first, rest = range(cuts // 2), range(cuts // 2, cuts)
    kind = jnp.where(par == 0, jnp.where(zi == hz - 1, 1, 0), jnp.where(zi == 0, 2, 3))

    def at_kinds(places, now, act):
        for q in range(4):
            if places[q] == now:
                @pl.when(kind == q)
                def _():
                    act()

    def partner(w, chunks):
        for c in chunks:
            w.to_partner(c).start()

    def mates(w):
        for j in range(1, hz):
            for c in every:
                w.to_mate(j, c).start()

    def issue(slot):
        at_kinds(PLAN["up_part"], slot, lambda: partner(up, every))
        at_kinds(PLAN["up_mate"], slot, lambda: mates(up))
        at_kinds(PLAN["dn_part0"], slot, lambda: partner(dn, first))
        at_kinds(PLAN["dn_part1"], slot, lambda: partner(dn, rest))
        at_kinds(PLAN["dn_mate"], slot, lambda: mates(dn))
        if slot > 0 and PLAN["own_y"][0] == slot:
            beside_y(dn)

    issue(0)
    local_up.start()
    local_dn.start()
    local_wout.start()

    def beside_y(w):
        for dy in range(1, ny):
            for c in every:
                w.own_y(dy, c).start()

    beside_y(up)
    if PLAN["own_y"][0] == 0:
        beside_y(dn)

    scale = hd ** (-0.5) * LOG2E

    def absorb(k, v, gates, diagonal):
        for h in range(heads):
            cols = pl.ds(h * hd, hd)
            rel = (gates[h:h + 1, :] - gate_ref[h:h + 1, 0:1]) * LOG2E
            s = lax.dot_general(q_ref[:, cols], k[:, cols], (((1,), (1,)), ((), ())),
                                preferred_element_type=jnp.float32)
            s = s * scale - rel
            if diagonal:
                qp = lax.broadcasted_iota(jnp.int32, s.shape, 0)
                kp = lax.broadcasted_iota(jnp.int32, s.shape, 1)
                s = jnp.where(kp <= qp, s, NEG)
            top = jnp.max(s, axis=1, keepdims=True)
            if not diagonal:
                old = m_s[:, h:h + 1]
                top = jnp.maximum(old, top)
                fade = jnp.exp2(old - top)
            w = jnp.exp2(s - top)
            total = jnp.sum(w, axis=1, keepdims=True)
            add = jnp.dot(w.astype(jnp.bfloat16), v[:, cols], preferred_element_type=jnp.float32)
            if not diagonal:
                total = l_s[:, h:h + 1] * fade + total
                add = acc_s[:, cols] * fade + add
            m_s[:, h:h + 1] = top
            l_s[:, h:h + 1] = total
            acc_s[:, cols] = add

    def partial(zq):
        for h in range(heads):
            cols = pl.ds(h * hd, hd)
            base = gate_ref[h:h + 1, 0:1] * LOG2E
            ss = []
            for i in range(ny):
                rel = g_all[i, h:h + 1, :] * LOG2E - base
                s = lax.dot_general(q_all[zq, :, cols], k_all[i, :, cols], (((1,), (1,)), ((), ())),
                                    preferred_element_type=jnp.float32)
                ss.append(s * scale - rel)
            top = jnp.max(functools.reduce(jnp.maximum, ss), axis=1, keepdims=True)
            total, add = 0.0, 0.0
            for i in range(ny):
                w = jnp.exp2(ss[i] - top)
                total += jnp.sum(w, axis=1, keepdims=True)
                add += jnp.dot(w.astype(jnp.bfloat16), v_all[i, :, cols], preferred_element_type=jnp.float32)
            o_send[zq, :, cols] = add.astype(jnp.bfloat16)
            st_s[:, h:h + 1] = top - base
            st_s[:, heads + h:heads + h + 1] = total
        stats = jnp.transpose(st_s[...])[0:STAT, :]
        t_send[zq] = stats
        t_own[pl.ds(pl.multiple_of(zq * STAT, STAT), STAT), :] = stats

    with jax.named_scope("diag"):
        absorb(k_ref, v_ref, gate_ref, True)

    for zq in range(2, nz):
        @pl.when((zq > z) & (z > 0))
        def _(zq=zq):
            for h in range(heads):
                with jax.named_scope("qfwd"):
                    query_wait(zq, h)
                query_on(zq, h).start()
    issue(1)

    for dy in range(1, ny):
        src = (y + dy) % ny

        @pl.when((z + 1 < nz) | (src < y))
        def _(dy=dy, src=src):
            with jax.named_scope("kvwait"):
                for ref, all_, ss, rs in ((k_ref, k_all, k_s, k_r), (gate_ref, g_all, g_s, g_r), (v_ref, v_all, v_s, v_r)):
                    rcopy(ref, all_.at[src], ss.at[0], rs.at[src], me).wait_recv()

            @pl.when(src < y)
            def _():
                with jax.named_scope("absorb"):
                    absorb(k_all.at[src], v_all.at[src], g_all.at[src], False)

    def query_level(i, carry):
        zq = i + 1

        @pl.when(zq > z)
        def _():
            @pl.when(z == 0)
            def _():
                with jax.named_scope("qwait"):
                    for h in range(heads):
                        query_wait(zq, h)
            with jax.named_scope("partial"):
                partial(zq)

            @pl.when(jnp.logical_not(merged(zq)))
            def _():
                part_do(zq, lambda c: c.start())
        return carry

    lax.fori_loop(0, nz - 1, query_level, 0)
    issue(2)

    for zq in range(hz, nz):
        @pl.when(merged(zq))
        def _(zq=zq):
            rows_at = pl.ds(zq * STAT, STAT)
            with jax.named_scope("midwait"):
                rcopy(o_send.at[0], o_mid.at[zq], o_s.at[0], om_r.at[zq], me).wait_recv()
                rcopy(t_send.at[0], t_mid.at[rows_at, :], t_s.at[0], tm_r.at[zq], me).wait_recv()
            t_own[0:STAT, :] = t_mid[rows_at, :]
            both = jnp.transpose(t_own[...])
            for h in range(heads):
                cols = pl.ds(h * hd, hd)
                at = zq * STAT + h
                m1, l1 = both[:, at:at + 1], both[:, at + heads:at + heads + 1]
                m2, l2 = both[:, h:h + 1], both[:, heads + h:heads + h + 1]
                top = jnp.maximum(m1, m2)
                f1, f2 = jnp.exp2(m1 - top), jnp.exp2(m2 - top)
                o_send[zq, :, cols] = (o_send[zq, :, cols].astype(jnp.float32) * f1
                                       + o_mid[zq, :, cols].astype(jnp.float32) * f2).astype(jnp.bfloat16)
                st_s[:, h:h + 1] = top
                st_s[:, heads + h:heads + h + 1] = l1 * f1 + l2 * f2
            t_send[zq] = jnp.transpose(st_s[...])[0:STAT, :]
            part_do(zq, lambda c: c.start())

    def serve(w, i, chunks, name):
        for c in chunks:
            with jax.named_scope(name):
                w.service(i, c)

    def up_mates():
        for j in range(1, hz):
            serve(up, j, every, "upsvc_mate")

    def early_up():
        serve(up, hz, every, "upsvc_part")

        at_kinds(PLAN["s_up_mate"], 0, up_mates)
        issue(3)
    def pass_on(when):
        at_kinds(PLAN["s_part0"], when, lambda: serve(dn, hz, first, "dnsvc_part0"))
        at_kinds(PLAN["s_part1"], when, lambda: serve(dn, hz, rest, "dnsvc_part1"))
        for j in range(1, hz):
            at_kinds(PLAN["s_mate"], when, lambda: serve(dn, j, every, "dnsvc_mate"))
            at_kinds(PLAN["s_far0"], when, lambda: serve(dn, hz + j, first, "dnsvc_far0"))

    @pl.when(z > 0)
    def _():
        early_up()

    for zk in range(nz - 1):
        @pl.when((zk < z) & ((par == 0) | (zk >= hz - 1)))
        def _(zk=zk):
            with jax.named_scope("owait"):
                at = pl.ds(zk * STAT, STAT)
                rcopy(o_send.at[0], o_recv.at[zk], o_s.at[0], o_r.at[zk], me).wait_recv()
                rcopy(t_send.at[0], t_recv.at[at, :], t_s.at[0], t_r.at[zk], me).wait_recv()

    @pl.when(z > 0)
    def _():
        st_s[...] = jnp.transpose(t_recv[...])

    for zk in range(nz - 1):
        @pl.when((zk < z) & ((par == 0) | (zk >= hz - 1)))
        def _(zk=zk):
            for h in range(heads):
                cols = pl.ds(h * hd, hd)
                at = zk * STAT + h
                their = st_s[:, at:at + 1] + gate_ref[h:h + 1, 0:1] * LOG2E
                old = m_s[:, h:h + 1]
                top = jnp.maximum(old, their)
                fade, rise = jnp.exp2(old - top), jnp.exp2(their - top)
                m_s[:, h:h + 1] = top
                l_s[:, h:h + 1] = l_s[:, h:h + 1] * fade + st_s[:, at + heads:at + heads + 1] * rise
                acc_s[:, cols] = acc_s[:, cols] * fade + o_recv[zk, :, cols].astype(jnp.float32) * rise

    for h in range(heads):
        cols = pl.ds(h * hd, hd)
        done = (acc_s[:, cols] / l_s[:, h:h + 1]).astype(jnp.bfloat16)
        for j in range(n_tp):
            att[j, :, cols] = done[j * rows:(j + 1) * rows, :]

    def heads_to(o):
        to = (tp + o) % n_tp
        return rcopy(att.at[to], att_in.at[tp], a_s.at[o], a_r.at[tp], me, to)

    for o in range(1, n_tp):
        heads_to(o).start()
    att_in[pl.ds(tp, 1)] = att[pl.ds(tp, 1)]
    local_wout.wait()
    with jax.named_scope("attwait"):
        for o in range(1, n_tp):
            src = (tp + o) % n_tp
            rcopy(att.at[0], att_in.at[src], a_s.at[0], a_r.at[src], me, tp).wait_recv()
    total = res_ref[...].astype(jnp.float32)
    for j in range(n_tp):
        total += jnp.dot(att_in[j], wout[j * width:(j + 1) * width, :], preferred_element_type=jnp.float32)
    rsum[...] = total
    mean_square = jnp.mean(total * total, axis=-1, keepdims=True)
    normed = (total * lax.rsqrt(mean_square + 1e-06) * gain_ref[...]).astype(jnp.bfloat16)

    def block(ref, b):
        at = (b % 2) * chips + b // 2
        return ref.at[pl.ds(pl.multiple_of(at * rows, rows), rows), :]

    block(norm_all, slot)[...] = normed
    strips = PLAN["strips"][0]
    strip = norm_all.shape[1] // strips

    def strip_of(b, c):
        at = (b % 2) * chips + b // 2
        return norm_all.at[pl.ds(pl.multiple_of(at * rows, rows), rows), pl.ds(c * strip, strip)]

    def normed_row(src, sem, other, c):
        sp_to, tp_to = place(other)
        return rcopy(strip_of(src, c), strip_of(src, c), n_s.at[sem * strips + c], n_r.at[src * strips + c], sp_to, tp_to)

    def beside(k):
        return par * n_tp + ((x + k) % cx) * 2 + core

    across = (1 - par) * n_tp + tp

    def normed_beside(k, c):
        return normed_row(slot, k, beside(k), c)

    def normed_across(c):
        return normed_row(slot, 0, across, c)

    def normed_relay(k, c):
        return normed_row(across, cx + k, beside(k), c)

    def normed_mate(k, c):
        return normed_row((slot + 2 * k) % group, chips + k, mate, c)

    def normed_wait(src, c):
        rcopy(strip_of(src, c), strip_of(src, c), n_s.at[0], n_r.at[src * strips + c], me).wait_recv()

    def gate(g):
        outer = jnp.where(par == 0, zi, hz - 1 - zi)
        for i in range(hz - 1):
            @pl.when(i < outer)
            def _(i=i):
                to = par * hz + jnp.where(par == 0, i, hz - 1 - i)
                for t in (tp, mate % n_tp):
                    pl.semaphore_signal(go.at[g], inc=1, device_id={"sp": to * ny + y, "tp": t},
                                        device_id_type=pl.DeviceIdType.MESH)
        pl.semaphore_signal(go.at[g], inc=1, device_id={"tp": mate % n_tp}, device_id_type=pl.DeviceIdType.MESH)
        with jax.named_scope("gate"):
            pl.semaphore_wait(go.at[g], 2 * (hz - 1 - outer) + 1)

    for c in range(strips):
        for k in range(1, cx):
            normed_beside(k, c).start()
    for c in range(strips):
        normed_mate(0, c).start()

    @pl.when(z == 0)
    def _():
        early_up()
    for zq in range(1, nz):
        @pl.when(zq > z)
        def _(zq=zq):
            with jax.named_scope("osent"):
                part_do(zq, lambda c: c.wait_send())
    if PLAN["gates"][0]:
        gate(0)
    issue(4)
    for c in range(strips):
        normed_across(c).start()
    issue(5)
    at_kinds(PLAN["s_up_mate"], 1, up_mates)
    pass_on(1)
    for j in range(1, hz):
        serve(up, hz + j, every, "upsvc_far")
    pass_on(2)

    for c in range(strips):
        with jax.named_scope("normwait_across"):
            normed_wait(across, c)
        for k in range(1, cx):
            normed_relay(k, c).start()
        normed_mate(chips // 2, c).start()
    with jax.named_scope("e2sent"):
        for c in range(strips):
            normed_across(c).wait_send()
    if PLAN["gates"][1]:
        gate(1)
    issue(6)
    pass_on(3)
    for near in (True, False):
        for k in range(1, cx):
            for c in range(strips):
                b = beside(k) if near else (1 - par) * n_tp + ((x + k) % cx) * 2 + core
                with jax.named_scope("normwait_chip"):
                    normed_wait(b, c)
                normed_row(b, chips + (b // 2 - mine + chips) % chips, mate, c).start()

    local_up.wait()
    with jax.named_scope("upwait_y"):
        for s in range(n_sp):
            @pl.when(s % ny != y)
            def _(s=s):
                for c in every:
                    up.wait(s, c)
    with jax.named_scope("normwait_mate"):
        for k in range(chips):
            for c in range(strips):
                normed_wait((mate + 2 * k) % group, c)

    tile = min(256, half)

    def up_tile(i, carry):
        cols = pl.ds(pl.multiple_of(i * tile, tile), tile)
        u = jnp.maximum(jnp.dot(norm_all[...], wu[:, cols], preferred_element_type=jnp.float32), 0.0)
        hid[:, cols] = (u * u).astype(jnp.bfloat16)
        return carry

    with jax.named_scope("up_mm"):
        lax.fori_loop(0, half // tile, up_tile, 0)

    per = max(1, 128 // cs)
    nk = ny // per
    span = per * cs

    def part(ref, at, count, c):
        return ref.at[pl.ds(pl.multiple_of(at * rows, rows), count * rows),
                      pl.ds(pl.multiple_of(c * span, span), span)]

    def to_mate(c):
        return rcopy(part(psend, (1 - core) * chips, chips, c), part(pmate, 0, chips, c),
                     x_s.at[c], x_r.at[c], me, mate % n_tp)

    def part_beside(k, pz, c):
        xd = (x + k) % cx
        return rcopy(part(pcomb, pz * cx + xd, 1, c), part(precv, x * 2 + pz, 1, c), p_s.at[(k * 2 + pz) * nz * nk + c],
                     p_r.at[(x * 2 + pz) * nz * nk + c], me, xd * 2 + core)

    def part_across(c):
        sp_to, tp_to = place(across)
        return rcopy(part(pfar, 0, 1, c), part(pback, 0, 1, c), f_s.at[c], f_r.at[c], sp_to, tp_to)

    def down_piece(c):
        ws = [wd[c * per + i] for i in range(per)]
        w = ws[0] if per == 1 else jnp.concatenate(ws, axis=1)
        cols = pl.ds(pl.multiple_of(c * span, span), span)
        m = hid.shape[0] // 2
        for a in range(2):
            psend[a * m:(a + 1) * m, cols] = jnp.dot(
                hid[a * m:(a + 1) * m, :], w, preferred_element_type=jnp.float32).astype(jnp.bfloat16)
        to_mate(c).start()

    def combine(c):
        with jax.named_scope("matewait"):
            to_mate(c).wait_recv()
        both = (part(psend, core * chips, chips, c)[...].astype(jnp.float32)
                + part(pmate, 0, chips, c)[...].astype(jnp.float32))
        part(pcomb, 0, chips, c)[...] = both.astype(jnp.bfloat16)
        for pz in range(2):
            for k in range(1, cx):
                part_beside(k, (1 - par + pz) % 2, c).start()

    def reduce(c):
        cols = pl.ds(pl.multiple_of(c * span, span), span)
        for far in (True, False):
            pz = 1 - par if far else par
            total = part(pcomb, pz * cx + x, 1, c)[...].astype(jnp.float32)
            for k in range(1, cx):
                xs = (x + k) % cx
                with jax.named_scope("besidewait"):
                    rcopy(part(pcomb, 0, 1, c), part(precv, xs * 2 + pz, 1, c), p_s.at[0],
                          p_r.at[(xs * 2 + pz) * nz * nk + c], me).wait_recv()
                total += part(precv, xs * 2 + pz, 1, c)[...].astype(jnp.float32)
            if far:
                pfar[:, cols] = total.astype(jnp.bfloat16)
                part_across(c).start()
            else:
                rsum[:, cols] += total

    def finish(c):
        cols = pl.ds(pl.multiple_of(c * span, span), span)
        with jax.named_scope("acrosswait"):
            part_across(c).wait_recv()
        out_ref[:, cols] = (rsum[:, cols] + pback[:, cols].astype(jnp.float32)).astype(jnp.bfloat16)

    local_dn.wait()

    pieces = []
    done = [0, 0]

    def flush(upto, summed):
        while done[0] < upto:
            combine(pieces[done[0]])
            done[0] += 1
        while done[1] < summed:
            reduce(pieces[done[1]])
            done[1] += 1

    def piece(i, k):
        c = dn.order(i) * nk + (y // per + k) % nk
        with jax.named_scope("dnwait_y"):
            for o in range(per):
                s = c * per + o

                @pl.when(s % ny != y)
                def _(s=s):
                    for cut in every:
                        dn.wait(s, cut)
        with jax.named_scope("down_mm"):
            down_piece(c)
        pieces.append(c)
        flush(len(pieces) - 1, len(pieces) - PLAN["lag"][0])

    for k in range(nk):
        piece(0, k)
    if PLAN["style"][0] == 0:
        pass_on(5)
    else:
        at_kinds(PLAN["s_part0"], 5, lambda: serve(dn, hz, first, "dnsvc_part0"))
        at_kinds(PLAN["s_part1"], 5, lambda: serve(dn, hz, rest, "dnsvc_part1"))
        piece(hz, 0)
    for j in range(1, hz):
        if PLAN["style"][0] == 1:
            at_kinds(PLAN["s_mate"], 5, lambda: serve(dn, j, every, "dnsvc_mate"))
            at_kinds(PLAN["s_far0"], 5, lambda: serve(dn, hz + j, first, "dnsvc_far0"))
        piece(j, 0)
    if PLAN["style"][0] == 0:
        piece(hz, 0)
    for j in range(1, hz):
        serve(dn, hz + j, rest, "dnsvc_far")
        if PLAN["style"][0] == 1:
            piece(hz + j, 0)
    for k in range(1, nk):
        for i in ([hz] + list(range(1, hz)) if PLAN["style"][0] == 1 else list(range(1, hz)) + [hz]):
            piece(i, k)
    for j in range(1, hz):
        for k in range(PLAN["style"][0], nk):
            piece(hz + j, k)
    flush(len(pieces), len(pieces))
    for c in pieces:
        finish(c)

    for dy in range(1, ny):
        @pl.when(keys_wanted(dy))
        def _(dy=dy):
            for c in keys_to(dy):
                c.wait_send()
    @pl.when(z > 0)
    def _():
        for h in range(heads):
            query_first(h).wait_send()
    for zq in range(2, nz):
        @pl.when((zq > z) & (z > 0))
        def _(zq=zq):
            for h in range(heads):
                query_on(zq, h).wait_send()
    up.drain()
    dn.drain()
    for o in range(1, n_tp):
        heads_to(o).wait_send()
    for c in range(strips):
        for k in range(1, cx):
            normed_beside(k, c).wait_send()
            normed_relay(k, c).wait_send()
        for k in range(chips):
            normed_mate(k, c).wait_send()
    for c in range(nz * nk):
        to_mate(c).wait_send()
        part_across(c).wait_send()
        for pz in range(2):
            for k in range(1, cx):
                part_beside(k, pz, c).wait_send()


def per_device(n_sp, n_tp, queries, keys, values, cum_gate, residual, w_out, gain, w_up, w_down):
    tok, width = queries.shape
    heads = cum_gate.shape[1]
    rows, features = residual.shape
    ny = n_tp // 2
    nz = n_sp // ny
    hz = nz // 2
    group = 2 * n_tp
    half = w_up.shape[1] // 2
    bf, f32 = jnp.bfloat16, jnp.float32
    assert nz % 2 == 0 and 2 * heads <= STAT
    gates = cum_gate.T
    vmem = pl.BlockSpec(memory_space=pltpu.VMEM)
    hbm = pl.BlockSpec(memory_space=pl.ANY)
    dma = lambda n: pltpu.SemaphoreType.DMA((n,))
    lanes = max(128, nz * STAT)
    pieces = nz * (ny // max(1, 128 // w_down.shape[1]))
    return pl.pallas_call(
        functools.partial(body, n_sp, n_tp, heads),
        out_shape=jax.ShapeDtypeStruct((rows, features), bf),
        in_specs=[vmem, vmem, vmem, vmem, vmem, hbm, vmem, hbm, hbm],
        out_specs=vmem,
        scratch_shapes=[
            pltpu.VMEM((nz, tok, width), bf),
            pltpu.VMEM((ny, tok, width), bf),
            pltpu.VMEM((ny, tok, width), bf),
            pltpu.VMEM((ny,) + gates.shape, f32),
            pltpu.VMEM((nz, tok, width), bf),
            pltpu.VMEM((nz, tok, width), bf),
            pltpu.VMEM((nz, STAT, tok), f32),
            pltpu.VMEM((lanes, tok), f32),
            pltpu.VMEM((nz, tok, width), bf),
            pltpu.VMEM((lanes, tok), f32),
            pltpu.VMEM((lanes, tok), f32),
            pltpu.VMEM((tok, lanes), f32),
            pltpu.VMEM((tok, 128), f32),
            pltpu.VMEM((tok, 128), f32),
            pltpu.VMEM((tok, width), f32),
            pltpu.VMEM((n_tp, rows, width), bf),
            pltpu.VMEM((n_tp, rows, width), bf),
            pltpu.VMEM(w_out.shape, bf),
            pltpu.VMEM((rows, features), f32),
            pltpu.VMEM((n_sp * w_up.shape[0], half), bf),
            pltpu.VMEM((n_sp, half, w_down.shape[1]), bf),
            pltpu.VMEM((group * rows, features), bf),
            pltpu.VMEM((group * rows, half), bf),
            pltpu.VMEM((group * rows, features), bf),
            pltpu.VMEM((n_tp * rows, features), bf),
            pltpu.VMEM((n_tp * rows, features), bf),
            pltpu.VMEM((n_tp * rows, features), bf),
            pltpu.VMEM((rows, features), bf),
            pltpu.VMEM((rows, features), bf),
        ]
        + [dma(nz * heads)] * 2 + [dma(ny)] * 6 + [dma(nz)] * 6
        + [dma(hz * PLAN["cuts"][0]), dma(hz * PLAN["cuts"][0]), dma(n_sp * PLAN["cuts"][0]), dma(n_sp * PLAN["cuts"][0])] * 2
        + [dma(n_tp), dma(n_tp), dma(PLAN["strips"][0] * group), dma(PLAN["strips"][0] * group)]
        + [dma(n_tp * pieces), dma(n_tp * pieces)] + [dma(pieces)] * 4 + [dma(3), pltpu.SemaphoreType.REGULAR((2,))],
        compiler_params=pltpu.CompilerParams(
            collective_id=0, has_side_effects=True, vmem_limit_bytes=63 * 1024 * 1024
        ),
    )(queries, keys, values, gates, residual, w_out, gain.reshape(1, -1), w_up, w_down)


def solution(mesh):
    n_sp, n_tp = mesh.shape["sp"], mesh.shape["tp"]
    return jax.shard_map(
        functools.partial(per_device, n_sp, n_tp),
        mesh=mesh,
        in_specs=(
            P("sp", "tp"),
            P("sp", "tp"),
            P("sp", "tp"),
            P("sp", "tp"),
            P(("sp", "tp"), None),
            P(),
            P(),
            P("sp", "tp"),
            P("tp", "sp"),
        ),
        out_specs=P(("sp", "tp"), None),
        check_vma=False,
    )
```
